32 devices in a mesh: sp: 16 (over z, y, x), tp: 2 (over core).
Axes of the slice: x: 2, y: 2, z: 4, core: 2. Of those that a mesh axis runs over, the one named last changes fastest.
Arguments:
- residual: bfloat16 [2048, 4096], P('tp', 'sp'), may hold values from -6 to 6
- values: bfloat16 [4096, 4096], P('sp', 'tp'), may hold values from -6 to 6
- gate_input: bfloat16 [4096, 4096], P('sp', 'tp'), may hold values from -6 to 6
- group_keys: bfloat16 [4096, 3072], P('sp', 'tp'), may hold values from -6 to 6
- time_step: float32 [64, 4096], P('tp', 'sp'), may hold values from -8 to 14
- decay_rate: float32 [64], P('tp'), may hold values from 0 to 2
- skip_gain: float32 [64], P('tp'), may hold values from 0.25 to 2
- conv_values: bfloat16 [4, 4096], P(None, 'tp'), may hold values from -3 to 3
- conv_keys: bfloat16 [4, 3072], P(None, 'tp'), may hold values from -3 to 3
- mix_gain: float32 [4096], P('tp'), may hold values from 0.1 to 1.9
- out_weight: bfloat16 [4096, 2048], P('tp'), may hold values from -0.09375 to 0.09375
- norm_gain: float32 [2048], replicated, may hold values from 0.1 to 1.9
- hidden_gate: bfloat16 [2048, 5120], P('sp', 'tp'), may hold values from -0.125 to 0.125
- hidden_up: bfloat16 [2048, 5120], P('sp', 'tp'), may hold values from -0.125 to 0.125
- hidden_conv: bfloat16 [2, 3, 5120], P(None, None, 'tp'), may hold values from -3.5 to 3.5
- hidden_down: bfloat16 [5120, 2048], P('tp', 'sp'), may hold values from -0.078125 to 0.078125
Outputs:
- layer_out: bfloat16 [2048, 4096], P('tp', 'sp')
The draws below stay inside these ranges and needn't reach their ends.
All inputs are finite; a program needn't handle non-finite values.
Results may differ from the reference program's by a relative error of at most 0.019.
Values may be sent and summed in bfloat16 or wider, within the bound.
A program may use at most 128 MiB of HBM per device.

```python
import math
import jax
import jax.numpy as jnp
from jax import lax

D = 2048
GROUPS = 8
GROUP_HEADS = 8
HEAD_SIZE = 64
STATE_WIDE = 128
STATE_NARROW = 64
FF = 5120
BLOCK = 128
SHORT_CONV = 4
HIDDEN_CONV = 3
TOK_DEV = 256
TOKENS = 4096
HEADS = 64
INNER = 4096
KEY_COLS = 3072
N_TP = 2


def draw_time_step(key, part):
    key_span = jax.random.fold_in(key, 101)
    key_block = jax.random.fold_in(key, 102)
    key_jitter = jax.random.fold_in(key, 103)
    span_count = TOKENS // TOK_DEV
    span_rank = jnp.arange(span_count, dtype=jnp.float32).reshape(span_count, 1)
    span_trend = 2.5 * (2.0 * span_rank / (span_count - 1) - 1.0)
    span_part = span_trend + jax.random.uniform(key_span, (span_count, 1), jnp.float32, -0.6, 0.6)
    span_part = jnp.broadcast_to(span_part, (span_count, TOK_DEV)).reshape(1, TOKENS)
    block_count = TOKENS // BLOCK
    block_part = jax.random.uniform(key_block, (block_count, 1), jnp.float32, -0.3, 0.3)
    block_part = jnp.broadcast_to(block_part, (block_count, BLOCK)).reshape(1, TOKENS)
    jitter = jnp.clip(0.5 * jax.random.normal(key_jitter, (HEADS, TOKENS), jnp.float32), -1.5, 1.5)
    log_step = math.log(0.1) + span_part + block_part + jitter
    return jnp.log(jnp.expm1(jnp.exp(log_step)))


def draw_decay_rate(key, part):
    key_pick = jax.random.fold_in(key, 201)
    key_fast = jax.random.fold_in(key, 202)
    key_slow = jax.random.fold_in(key, 203)
    fast_share = 0.5
    picked = jax.random.uniform(key_pick, (HEADS,), jnp.float32) < fast_share
    fast_rate = jnp.exp(jax.random.uniform(key_fast, (HEADS,), jnp.float32, math.log(0.1), math.log(0.32)))
    slow_rate = jnp.exp(jax.random.uniform(key_slow, (HEADS,), jnp.float32, math.log(0.3), math.log(4.0))) / TOKENS
    return jnp.where(picked, fast_rate, slow_rate)


def levels(rng, shape, shards, low, largest):
    factor_of, own = 1.0, jax.random.fold_in(rng, 6)
    for position, blocks in shards:
        heights = jnp.exp(jax.random.uniform(jax.random.fold_in(own, position), (blocks,), jnp.float32, low / len(shards), largest / len(shards)))
        factor_of = factor_of * jnp.repeat(heights, shape[position] // blocks).reshape([-1 if axis == position else 1 for axis in range(len(shape))])
    return factor_of


def normal_values(rng, shape, width, reach, split=(), held_as=jnp.bfloat16):
    loudness = levels(rng, shape, split, -0.22, 0.18) if split else 1.0
    drawn = jax.random.normal(rng, shape, jnp.float32) * width * loudness
    return jnp.minimum(jnp.maximum(drawn, -reach), reach).astype(held_as)


def setup_inputs(seed: int = 0) -> dict:
    streams_of = jax.random.split(jax.random.key(seed), 17)
    residual = normal_values(streams_of[0], (D, TOKENS), 1.0, 6.0, ((0, 2), (1, 16)))
    values = normal_values(streams_of[1], (TOKENS, INNER), 1.0, 6.0, ((0, 16), (1, 2)))
    gate_input = normal_values(streams_of[2], (TOKENS, INNER), 1.0, 6.0, ((0, 16), (1, 2)))
    group_keys = normal_values(streams_of[3], (TOKENS, KEY_COLS), 1.0, 6.0, ((0, 16), (1, 2)))
    time_step = draw_time_step(jax.random.fold_in(streams_of[16], 71), 0)
    decay_rate = draw_decay_rate(jax.random.fold_in(streams_of[16], 71), 0)
    skip_gain = jnp.clip(jnp.exp(math.log(2.0) - 2.0794415 * jax.random.uniform(streams_of[6], (HEADS,), jnp.float32) ** levels(streams_of[6], (HEADS,), ((0, 2),), -0.2, 0.2)), 0.25, 2.0)
    conv_values = normal_values(streams_of[7], (SHORT_CONV, INNER), SHORT_CONV ** -0.5, 3.0, ((1, 2),))
    conv_keys = normal_values(streams_of[8], (SHORT_CONV, KEY_COLS), SHORT_CONV ** -0.5, 3.0, ((1, 2),))
    mix_gain = jnp.clip(1.0 + 0.18 * jax.random.normal(streams_of[9], (INNER,), jnp.float32), 0.1, 1.9)
    out_weight = normal_values(streams_of[10], (INNER, D), INNER ** -0.5, 0.09375, ((0, 2),))
    norm_gain = jnp.clip(1.0 + 0.18 * jax.random.normal(streams_of[11], (D,), jnp.float32), 0.1, 1.9)
    hidden_gate = normal_values(streams_of[12], (D, FF), D ** -0.5, 0.125, ((0, 16), (1, 2)))
    hidden_up = normal_values(streams_of[13], (D, FF), D ** -0.5, 0.125, ((0, 16), (1, 2)))
    hidden_conv = normal_values(streams_of[14], (2, HIDDEN_CONV, FF), HIDDEN_CONV ** -0.5, 3.5, ((2, 2),))
    hidden_down = normal_values(streams_of[15], (FF, D), FF ** -0.5, 0.078125, ((0, 2), (1, 16)))
    return dict(residual=residual, values=values, gate_input=gate_input, group_keys=group_keys, time_step=time_step, decay_rate=decay_rate, skip_gain=skip_gain, conv_values=conv_values, conv_keys=conv_keys, mix_gain=mix_gain, out_weight=out_weight, norm_gain=norm_gain, hidden_gate=hidden_gate, hidden_up=hidden_up, hidden_conv=hidden_conv, hidden_down=hidden_down)


NORM_FLOOR = 0.1
HIGHEST = lax.Precision.HIGHEST

def causal_taps(padded, weights, first_row, row_count):
    tap_count = weights.shape[0]
    window = lax.dynamic_slice_in_dim(padded, first_row, row_count + tap_count - 1, 0).astype(jnp.float32)
    summed = weights[0].astype(jnp.float32) * window[0:row_count]
    for tap_index in range(1, tap_count):
        summed = summed + weights[tap_index].astype(jnp.float32) * window[tap_index:tap_index + row_count]
    return summed

def block_heads(inputs, in_keys, out_keys, deltas, decay_rates, skip_table, carried):
    length = inputs.shape[0]
    running = jnp.cumsum(-decay_rates * deltas, axis=0)
    weighted = inputs * deltas[..., None]
    scores = jnp.einsum('ign,jgn->gij', out_keys, in_keys, precision=HIGHEST)
    by_head = jnp.transpose(running, (1, 2, 0))
    between = by_head[..., :, None] - by_head[..., None, :]
    lower_mask = jnp.tril(jnp.ones((length, length), dtype=bool))
    decays = jnp.exp(jnp.where(lower_mask, between, -jnp.inf))
    inside = jnp.einsum('ghij,jghp->ighp', scores[:, None] * decays, weighted, precision=HIGHEST)
    carried_part = jnp.einsum('ign,ghpn->ighp', out_keys, carried, precision=HIGHEST) * jnp.exp(running)[..., None]
    to_end = jnp.exp(by_head[..., -1:] - by_head)
    fresh_state = jnp.einsum('jgn,ghj,jghp->ghpn', in_keys, to_end, weighted, precision=HIGHEST)
    updated = carried * jnp.exp(by_head[..., -1])[..., None, None] + fresh_state
    return (inside + carried_part + inputs * skip_table[..., None], updated)

def sharded_sum(base, left, right, shard_count):
    share = left.shape[1] // shard_count
    summed = base
    for shard in range(shard_count):
        partial_out = jnp.dot(left[:, shard * share:(shard + 1) * share], right[shard * share:(shard + 1) * share], preferred_element_type=jnp.float32)
        partial_out = lax.optimization_barrier(partial_out.astype(jnp.bfloat16))
        summed = summed + partial_out.astype(jnp.float32)
    return summed

def reference(residual, values, gate_input, group_keys, time_step, decay_rate, skip_gain, conv_values, conv_keys, mix_gain, out_weight, norm_gain, hidden_gate, hidden_up, hidden_conv, hidden_down):
    tap_count = conv_values.shape[0]
    pad_values = jnp.pad(values, ((tap_count - 1, 0), (0, 0)))
    pad_keys = jnp.pad(group_keys, ((tap_count - 1, 0), (0, 0)))
    all_deltas = jax.nn.softplus(time_step)
    half_heads = GROUP_HEADS // 2
    wide_end = 2 * STATE_WIDE
    rate_table = decay_rate.reshape(GROUPS, GROUP_HEADS)
    skip_table = skip_gain.reshape(GROUPS, GROUP_HEADS)

    def one_block(carries, block_index):
        first_row = block_index * BLOCK
        inputs = jax.nn.silu(causal_taps(pad_values, conv_values, first_row, BLOCK)).reshape(BLOCK, GROUPS, GROUP_HEADS, HEAD_SIZE)
        key_rows = jax.nn.silu(causal_taps(pad_keys, conv_keys, first_row, BLOCK)).reshape(BLOCK, GROUPS, -1)
        deltas = lax.dynamic_slice_in_dim(all_deltas, first_row, BLOCK, 1).T.reshape(BLOCK, GROUPS, GROUP_HEADS)
        wide_out, wide_state = block_heads(inputs[:, :, :half_heads], key_rows[..., :STATE_WIDE], key_rows[..., STATE_WIDE:wide_end], deltas[:, :, :half_heads], rate_table[:, :half_heads], skip_table[:, :half_heads], carries[0])
        narrow_out, narrow_state = block_heads(inputs[:, :, half_heads:], key_rows[..., wide_end:wide_end + STATE_NARROW], key_rows[..., wide_end + STATE_NARROW:], deltas[:, :, half_heads:], rate_table[:, half_heads:], skip_table[:, half_heads:], carries[1])
        mixer_out = jnp.concatenate([wide_out, narrow_out], axis=2).reshape(BLOCK, INNER)
        gate_rows = lax.dynamic_slice_in_dim(gate_input, first_row, BLOCK, 0).astype(jnp.float32)
        gated_out = mixer_out * jax.nn.silu(gate_rows)
        inverse_rms = lax.rsqrt(lax.optimization_barrier(jnp.mean(gated_out * gated_out, axis=1, keepdims=True)) + NORM_FLOOR)
        normed = (gated_out * inverse_rms * mix_gain).astype(jnp.bfloat16)
        return ((wide_state, narrow_state), normed)
    start_state = (jnp.zeros((GROUPS, half_heads, HEAD_SIZE, STATE_WIDE), jnp.float32), jnp.zeros((GROUPS, GROUP_HEADS - half_heads, HEAD_SIZE, STATE_NARROW), jnp.float32))
    final_state, normed_blocks = lax.scan(one_block, start_state, jnp.arange(TOKENS // BLOCK, dtype=jnp.int32))
    normed_all = normed_blocks.reshape(TOKENS, INNER)
    merged = sharded_sum(residual.T.astype(jnp.float32), normed_all, out_weight, N_TP).astype(jnp.bfloat16)
    merged_wide = merged.astype(jnp.float32)
    inverse_norm = lax.rsqrt(lax.optimization_barrier(jnp.mean(merged_wide * merged_wide, axis=1, keepdims=True)) + NORM_FLOOR)
    lifted = (merged_wide * inverse_norm * norm_gain).astype(jnp.bfloat16)
    gate_pre = jnp.dot(lifted, hidden_gate, preferred_element_type=jnp.float32).astype(jnp.bfloat16)
    up_pre = jnp.dot(lifted, hidden_up, preferred_element_type=jnp.float32).astype(jnp.bfloat16)
    edge_count = hidden_conv.shape[1] - 1
    gate_conv = causal_taps(jnp.pad(gate_pre, ((edge_count, 0), (0, 0))), hidden_conv[0], 0, TOKENS)
    up_conv = causal_taps(jnp.pad(up_pre, ((edge_count, 0), (0, 0))), hidden_conv[1], 0, TOKENS)
    hidden = (jax.nn.silu(gate_conv) * up_conv).astype(jnp.bfloat16)
    layer_out = sharded_sum(merged_wide, hidden, hidden_down, N_TP).astype(jnp.bfloat16)
    return layer_out.T
```

```python
import jax
import jax.numpy as jnp
from jax import lax
from jax.sharding import PartitionSpec as P

GROUP_HEADS = 8
HEAD_SIZE = 64
STATE_WIDE = 128
STATE_NARROW = 64
BLOCK = 128


NORM_FLOOR = 0.1
SPAN = 4
HIGHEST = lax.Precision.HIGHEST


def from_behind(value, axis, steps):
    count = lax.axis_size(axis)
    first, last = (max(0, -steps), min(count, count - steps))
    return lax.ppermute(value, axis, [(source, source + steps) for source in range(first, last)])


def earlier_states(log_spans, states, axis):
    count = lax.axis_size(axis)
    place = lax.axis_index(axis)
    slices = []
    for state in states:
        heads, size, width = state.shape
        cut = state.astype(jnp.bfloat16).reshape(heads, count, size // count * width)
        slices.append(jnp.transpose(cut, (1, 0, 2)).reshape(count, -1))
    split = slices[0].shape[1]
    sent = jnp.concatenate(slices, axis=1)
    got = lax.all_to_all(sent, axis, split_axis=0, concat_axis=0, tiled=True)
    spans = lax.all_gather(log_spans, axis)
    spot = jnp.arange(count)
    between = (spot[None, :, None] < spot) & (spot < spot[:, None, None])
    gaps = jnp.einsum("dsr,rh->dsh", between.astype(jnp.float32), spans, precision=HIGHEST)
    earlier = jnp.tril(jnp.ones((count, count), dtype=bool), -1)
    factors = jnp.exp(jnp.where(earlier[..., None], gaps, -jnp.inf))
    first = 0
    backs = []
    for state, part in zip(states, (got[:, :split], got[:, split:])):
        heads, size, width = state.shape
        rows = part.reshape(count, heads, size // count * width)
        mine = factors[:, :, first : first + heads]
        first += heads
        backs.append(
            jnp.einsum("dsh,shn->dhn", mine.astype(jnp.bfloat16), rows, preferred_element_type=jnp.float32)
            .astype(jnp.bfloat16)
            .reshape(count, -1)
        )
    back = lax.all_to_all(
        jnp.concatenate(backs, axis=1), axis, split_axis=0, concat_axis=0, tiled=True
    )
    results = []
    for state, part in zip(states, (back[:, :split], back[:, split:])):
        heads, size, width = state.shape
        rows = part.reshape(count, heads, size // count, width)
        results.append(jnp.transpose(rows, (1, 0, 2, 3)).reshape(heads, size, width))
    return results


def from_member(shard, axis, span, turn):
    count = lax.axis_size(axis)
    return lax.ppermute(
        shard, axis, [(i, i - i % span + (i + turn) % span) for i in range(count)]
    )


def with_tp_sum(partial, rows):
    count = lax.axis_size("tp")
    place = lax.axis_index("tp")
    total = lax.dynamic_slice_in_dim(partial, place * rows, rows, 0).astype(jnp.float32)
    for turn in range(1, count):
        block = lax.dynamic_slice_in_dim(partial, (place + turn) % count * rows, rows, 0)
        total = total + from_member(block, "tp", count, turn).astype(jnp.float32)
    return total


def tap_sum(joined, weights, row_count):
    summed = weights[0].astype(jnp.float32) * joined[0:row_count]
    for tap_index in range(1, weights.shape[0]):
        summed = (
            summed
            + weights[tap_index].astype(jnp.float32) * joined[tap_index : tap_index + row_count]
        )
    return summed


def block_heads(inputs, in_keys, out_keys, deltas, decay_rates, skip_table, carried):
    length = inputs.shape[0]
    running = jnp.cumsum(-decay_rates * deltas, axis=0)
    weighted = inputs * deltas[..., None]
    scores = jnp.einsum("ign,jgn->gij", out_keys, in_keys, precision=HIGHEST)
    by_head = jnp.transpose(running, (1, 2, 0))
    between = by_head[..., :, None] - by_head[..., None, :]
    lower_mask = jnp.tril(jnp.ones((length, length), dtype=bool))
    decays = jnp.exp(jnp.where(lower_mask, between, -jnp.inf))
    inside = jnp.einsum("ghij,jghp->ighp", scores[:, None] * decays, weighted, precision=HIGHEST)
    carried_part = (
        jnp.einsum("ign,ghpn->ighp", out_keys, carried, precision=HIGHEST)
        * jnp.exp(running)[..., None]
    )
    to_end = jnp.exp(by_head[..., -1:] - by_head)
    fresh_state = jnp.einsum("jgn,ghj,jghp->ghpn", in_keys, to_end, weighted, precision=HIGHEST)
    updated = carried * jnp.exp(by_head[..., -1])[..., None, None] + fresh_state
    return (inside + carried_part + inputs * skip_table[..., None], updated)


def contract_rows(left, right):
    return lax.dot_general(
        left, right, (((0,), (0,)), ((), ())), preferred_element_type=jnp.float32
    )


def combine_states(first_part, second_part):
    return (
        first_part[0] * second_part[0],
        first_part[1] * second_part[0][..., None, None] + second_part[1],
        first_part[2] * second_part[2],
        first_part[3] * second_part[2][..., None, None] + second_part[3],
    )


def hidden_taps(both_pre, edge_cols, taps, row_count):
    joined_hidden = jnp.concatenate([edge_cols, both_pre], axis=2).astype(jnp.float32)
    conv_total = taps[:, 0, :, None].astype(jnp.float32) * joined_hidden[:, :, 0:row_count]
    for tap_index in range(1, taps.shape[1]):
        conv_total = (
            conv_total
            + taps[:, tap_index, :, None].astype(jnp.float32)
            * joined_hidden[:, :, tap_index : tap_index + row_count]
        )
    return (jax.nn.silu(conv_total[0]) * conv_total[1]).astype(jnp.bfloat16)


def hidden_weights(hidden_gate, hidden_up, hidden_down, span):
    count = lax.axis_size("sp")
    rows, hidden_cols = hidden_gate.shape
    quarter = hidden_cols // span
    within = [[g * span + m for m in range(span)] for g in range(count // span)]
    across = [[g * span + m for g in range(count // span)] for m in range(span)]
    gates = hidden_gate.reshape(rows, span, quarter)
    ups = hidden_up.reshape(rows, span, quarter)
    both = jnp.transpose(jnp.concatenate([gates, ups], axis=2), (1, 0, 2))
    down = hidden_down.reshape(span, quarter, hidden_down.shape[1])
    both = lax.all_to_all(both, "sp", 0, 0, axis_index_groups=within, tiled=True)
    down = lax.all_to_all(down, "sp", 0, 0, axis_index_groups=within, tiled=True)
    both = lax.all_gather(
        both.reshape(span * rows, 2 * quarter), "sp", axis_index_groups=across, tiled=True
    )
    down = lax.all_gather(down, "sp", axis_index_groups=across, tiled=True)
    down = jnp.transpose(down, (1, 0, 2)).reshape(quarter, -1)
    return both, down


def local(
    residual,
    values,
    gate_input,
    group_keys,
    time_step,
    decay_rate,
    skip_gain,
    conv_values,
    conv_keys,
    mix_gain,
    out_weight,
    norm_gain,
    hidden_gate,
    hidden_up,
    hidden_conv,
    hidden_down,
):
    row_count = values.shape[0]
    value_cols = values.shape[1]
    tap_count = conv_values.shape[0]
    sp_count = lax.axis_size("sp")
    span = min(SPAN, sp_count)
    member = lax.axis_index("sp") % span
    both_weights, down_quarter = hidden_weights(hidden_gate, hidden_up, hidden_down, span)
    quarter = down_quarter.shape[0]
    tail_rows = jnp.concatenate(
        [values[row_count - tap_count + 1 :], group_keys[row_count - tap_count + 1 :]], axis=1
    )
    before_rows = from_behind(tail_rows, "sp", 1)
    joined_values = jnp.concatenate([before_rows[:, :value_cols], values], axis=0).astype(
        jnp.float32
    )
    joined_keys = jnp.concatenate([before_rows[:, value_cols:], group_keys], axis=0).astype(
        jnp.float32
    )
    group_count = group_keys.shape[1] // (2 * STATE_WIDE + 2 * STATE_NARROW)
    inputs = jax.nn.silu(tap_sum(joined_values, conv_values, row_count)).reshape(
        row_count, group_count, GROUP_HEADS, HEAD_SIZE
    )
    key_rows = jax.nn.silu(tap_sum(joined_keys, conv_keys, row_count)).reshape(
        row_count, group_count, -1
    )
    deltas = jax.nn.softplus(time_step).T.reshape(row_count, group_count, GROUP_HEADS)
    rate_table = decay_rate.reshape(group_count, GROUP_HEADS)
    skip_table = skip_gain.reshape(group_count, GROUP_HEADS)
    running = jnp.cumsum(-rate_table * deltas, axis=0)
    half_heads = GROUP_HEADS // 2
    wide_end = 2 * STATE_WIDE

    def run_kind(head_first, head_last, key_first, state_width):
        in_keys = key_rows[..., key_first : key_first + state_width]
        out_keys = key_rows[..., key_first + state_width : key_first + 2 * state_width]
        carried = jnp.zeros(
            (group_count, head_last - head_first, HEAD_SIZE, state_width), jnp.float32
        )
        block_outs = []
        for block_index in range(row_count // BLOCK):
            row_first = block_index * BLOCK
            row_last = row_first + BLOCK
            block_out, carried = block_heads(
                inputs[row_first:row_last, :, head_first:head_last],
                in_keys[row_first:row_last],
                out_keys[row_first:row_last],
                deltas[row_first:row_last, :, head_first:head_last],
                rate_table[:, head_first:head_last],
                skip_table[:, head_first:head_last],
                carried,
            )
            block_outs.append(block_out)
        return (jnp.concatenate(block_outs, axis=0), carried, out_keys)

    wide_local, wide_state, wide_keys = run_kind(0, half_heads, 0, STATE_WIDE)
    narrow_local, narrow_state, narrow_keys = run_kind(
        half_heads, GROUP_HEADS, wide_end, STATE_NARROW
    )
    incoming = earlier_states(
        jnp.concatenate(
            [running[-1][:, :half_heads].reshape(-1), running[-1][:, half_heads:].reshape(-1)]
        ),
        (
            wide_state.reshape(-1, HEAD_SIZE, STATE_WIDE),
            narrow_state.reshape(-1, HEAD_SIZE, STATE_NARROW),
        ),
        "sp",
    )
    wide_in = incoming[0].reshape(wide_state.shape).astype(jnp.float32)
    narrow_in = incoming[1].reshape(narrow_state.shape).astype(jnp.float32)
    growth = jnp.exp(running)[..., None]
    wide_out = (
        wide_local
        + jnp.einsum("ign,ghpn->ighp", wide_keys, wide_in, precision=HIGHEST)
        * growth[:, :, :half_heads]
    )
    narrow_out = (
        narrow_local
        + jnp.einsum("ign,ghpn->ighp", narrow_keys, narrow_in, precision=HIGHEST)
        * growth[:, :, half_heads:]
    )
    mixer_out = jnp.concatenate([wide_out, narrow_out], axis=2).reshape(row_count, value_cols)
    gated_out = mixer_out * jax.nn.silu(gate_input.astype(jnp.float32))
    squares = lax.psum(jnp.sum(gated_out * gated_out, axis=1), "tp")
    inverse_rms = lax.rsqrt(squares / (value_cols * lax.axis_size("tp")) + NORM_FLOOR)
    gained = (gated_out * mix_gain).astype(jnp.bfloat16)
    mixer_part = lax.dot_general(
        out_weight, gained, (((0,), (1,)), ((), ())), preferred_element_type=jnp.float32
    ).astype(jnp.bfloat16)
    own_rows = residual.shape[0]
    mixer_sum = with_tp_sum(mixer_part, own_rows) * inverse_rms[None, :]
    own_merged = (residual.astype(jnp.float32) + mixer_sum).astype(jnp.bfloat16)
    pieces = [own_merged]
    for turn in range(1, span):
        pieces.append(from_member(own_merged, "sp", span, turn))
    mine = jnp.concatenate(pieces, axis=1)
    merged = lax.all_gather(mine, "tp", axis=0, tiled=True)
    merged_wide = merged.astype(jnp.float32)
    inverse_norm = lax.rsqrt(jnp.mean(merged_wide * merged_wide, axis=0) + NORM_FLOOR)
    lifted = (merged_wide * inverse_norm[None, :] * norm_gain[:, None]).astype(jnp.bfloat16)
    both_pre = contract_rows(both_weights, lifted).astype(jnp.bfloat16)
    edge_taps = hidden_conv.shape[1]
    both_pre = both_pre.reshape(2, quarter, span * row_count)
    ordered = [both_pre[:, :, j * row_count : (j + 1) * row_count] for j in range(span)]
    last_edges = [block[:, :, row_count - edge_taps + 1 :] for block in ordered]
    own_last = sum(
        jnp.where(member == (span - 1 + j) % span, 1, 0).astype(jnp.bfloat16) * last_edges[j]
        for j in range(span)
    )
    edge_before = from_behind(own_last, "sp", span)
    own_taps = lax.dynamic_slice_in_dim(hidden_conv, member * quarter, quarter, 2)
    hidden_blocks = []
    for j in range(span):
        first = member == j
        edge = jnp.where(first, edge_before, last_edges[(j + 1) % span])
        hidden_blocks.append(hidden_taps(ordered[j], edge, own_taps, row_count))
    hidden = jnp.concatenate(hidden_blocks, axis=1)
    down_part = contract_rows(down_quarter, hidden).astype(jnp.bfloat16)
    down_sum = with_tp_sum(down_part, own_rows)
    total = own_merged.astype(jnp.float32) + down_sum[:, :row_count]
    for turn in range(1, span):
        block = down_sum[:, turn * row_count : (turn + 1) * row_count].astype(jnp.bfloat16)
        total = total + from_member(block, "sp", span, span - turn).astype(jnp.float32)
    return total.astype(jnp.bfloat16)


def solution(mesh):
    in_specs = (
        P("tp", "sp"),
        P("sp", "tp"),
        P("sp", "tp"),
        P("sp", "tp"),
        P("tp", "sp"),
        P("tp"),
        P("tp"),
        P(None, "tp"),
        P(None, "tp"),
        P("tp"),
        P("tp", None),
        P(),
        P("sp", "tp"),
        P("sp", "tp"),
        P(None, None, "tp"),
        P("tp", "sp"),
    )
    out_specs = P("tp", "sp")
    return jax.shard_map(local, mesh=mesh, in_specs=in_specs, out_specs=out_specs, check_vma=False)
```

```python
import jax
import jax.numpy as jnp
from jax import lax
from jax.sharding import PartitionSpec as P

GROUP_HEADS = 8
HEAD_SIZE = 64
STATE_WIDE = 128
STATE_NARROW = 64
BLOCK = 128


NORM_FLOOR = 0.1
SPAN = 4
HIGHEST = lax.Precision.HIGHEST


def from_behind(value, axis, steps):
    count = lax.axis_size(axis)
    first, last = (max(0, -steps), min(count, count - steps))
    return lax.ppermute(value, axis, [(source, source + steps) for source in range(first, last)])


def earlier_states(log_spans, states, axis):
    count = lax.axis_size(axis)
    place = lax.axis_index(axis)
    slices = []
    for state in states:
        heads, size, width = state.shape
        cut = state.astype(jnp.bfloat16).reshape(heads, count, size // count * width)
        slices.append(jnp.transpose(cut, (1, 0, 2)).reshape(count, -1))
    split = slices[0].shape[1]
    high = lax.reduce_precision(log_spans, 8, 7)
    middle = lax.reduce_precision(log_spans - high, 8, 7)
    low = lax.reduce_precision(log_spans - high - middle, 8, 7)
    parts = jnp.concatenate([high, middle, low]).astype(jnp.bfloat16)
    slices.append(jnp.broadcast_to(parts, (count, parts.shape[0])))
    last = split + slices[1].shape[1]
    sent = jnp.concatenate(slices, axis=1)
    got = lax.all_to_all(sent, axis, split_axis=0, concat_axis=0, tiled=True)
    spans = got[:, last:].astype(jnp.float32).reshape(count, 3, -1).sum(axis=1)
    spot = jnp.arange(count)
    between = (spot[None, :, None] < spot) & (spot < spot[:, None, None])
    gaps = jnp.einsum("dsr,rh->dsh", between.astype(jnp.float32), spans, precision=HIGHEST)
    earlier = jnp.tril(jnp.ones((count, count), dtype=bool), -1)
    factors = jnp.exp(jnp.where(earlier[..., None], gaps, -jnp.inf))
    first = 0
    backs = []
    for state, part in zip(states, (got[:, :split], got[:, split:last])):
        heads, size, width = state.shape
        rows = part.reshape(count, heads, size // count * width)
        mine = factors[:, :, first : first + heads]
        first += heads
        backs.append(
            jnp.einsum("dsh,shn->dhn", mine.astype(jnp.bfloat16), rows, preferred_element_type=jnp.float32)
            .astype(jnp.bfloat16)
            .reshape(count, -1)
        )
    back = lax.all_to_all(
        jnp.concatenate(backs, axis=1), axis, split_axis=0, concat_axis=0, tiled=True
    )
    results = []
    for state, part in zip(states, (back[:, :split], back[:, split:])):
        heads, size, width = state.shape
        rows = part.reshape(count, heads, size // count, width)
        results.append(jnp.transpose(rows, (1, 0, 2, 3)).reshape(heads, size, width))
    return results


def from_member(shard, axis, span, turn):
    count = lax.axis_size(axis)
    return lax.ppermute(
        shard, axis, [(i, i - i % span + (i + turn) % span) for i in range(count)]
    )


def with_tp_sum(partial, rows):
    count = lax.axis_size("tp")
    place = lax.axis_index("tp")
    total = lax.dynamic_slice_in_dim(partial, place * rows, rows, 0).astype(jnp.float32)
    for turn in range(1, count):
        block = lax.dynamic_slice_in_dim(partial, (place + turn) % count * rows, rows, 0)
        total = total + from_member(block, "tp", count, turn).astype(jnp.float32)
    return total


def tap_sum(joined, weights, row_count):
    summed = weights[0].astype(jnp.float32) * joined[0:row_count]
    for tap_index in range(1, weights.shape[0]):
        summed = (
            summed
            + weights[tap_index].astype(jnp.float32) * joined[tap_index : tap_index + row_count]
        )
    return summed


def gathered_tp(mine):
    count = lax.axis_size("tp")
    if count > 2:
        return lax.all_gather(mine, "tp", axis=0, tiled=True)
    other = from_member(mine, "tp", count, 1)
    first = lax.axis_index("tp") == 0
    return jnp.concatenate([jnp.where(first, mine, other), jnp.where(first, other, mine)], axis=0)


def block_heads(inputs, in_keys, out_keys, deltas, decay_rates, skip_table, carried):
    length = inputs.shape[0]
    running = jnp.cumsum(-decay_rates * deltas, axis=0)
    weighted = inputs * deltas[..., None]
    scores = jnp.einsum("ign,jgn->gij", out_keys, in_keys, precision=HIGHEST)
    by_head = jnp.transpose(running, (1, 2, 0))
    between = by_head[..., :, None] - by_head[..., None, :]
    lower_mask = jnp.tril(jnp.ones((length, length), dtype=bool))
    decays = jnp.exp(jnp.where(lower_mask, between, -jnp.inf))
    inside = jnp.einsum("ghij,jghp->ighp", scores[:, None] * decays, weighted, precision=HIGHEST)
    carried_part = (
        jnp.einsum("ign,ghpn->ighp", out_keys, carried, precision=HIGHEST)
        * jnp.exp(running)[..., None]
    )
    to_end = jnp.exp(by_head[..., -1:] - by_head)
    fresh_state = jnp.einsum("jgn,ghj,jghp->ghpn", in_keys, to_end, weighted, precision=HIGHEST)
    updated = carried * jnp.exp(by_head[..., -1])[..., None, None] + fresh_state
    return (inside + carried_part + inputs * skip_table[..., None], updated)


def contract_rows(left, right):
    return lax.dot_general(
        left, right, (((0,), (0,)), ((), ())), preferred_element_type=jnp.float32
    )


def combine_states(first_part, second_part):
    return (
        first_part[0] * second_part[0],
        first_part[1] * second_part[0][..., None, None] + second_part[1],
        first_part[2] * second_part[2],
        first_part[3] * second_part[2][..., None, None] + second_part[3],
    )


def hidden_taps(both_pre, edge_cols, taps, row_count):
    joined_hidden = jnp.concatenate([edge_cols, both_pre], axis=2).astype(jnp.float32)
    conv_total = taps[:, 0, :, None].astype(jnp.float32) * joined_hidden[:, :, 0:row_count]
    for tap_index in range(1, taps.shape[1]):
        conv_total = (
            conv_total
            + taps[:, tap_index, :, None].astype(jnp.float32)
            * joined_hidden[:, :, tap_index : tap_index + row_count]
        )
    return (jax.nn.silu(conv_total[0]) * conv_total[1]).astype(jnp.bfloat16)


def hidden_weights(hidden_gate, hidden_up, hidden_down, span):
    count = lax.axis_size("sp")
    rows, hidden_cols = hidden_gate.shape
    quarter = hidden_cols // span
    within = [[g * span + m for m in range(span)] for g in range(count // span)]
    gates = hidden_gate.reshape(rows, span, quarter)
    ups = hidden_up.reshape(rows, span, quarter)
    both = jnp.transpose(jnp.concatenate([gates, ups], axis=2), (1, 0, 2))
    down = hidden_down.reshape(span, quarter, hidden_down.shape[1])
    both = lax.all_to_all(both, "sp", 0, 0, axis_index_groups=within, tiled=True)
    down = lax.all_to_all(down, "sp", 0, 0, axis_index_groups=within, tiled=True)
    return both.reshape(span * rows, 2 * quarter), down


def gathered_weights(both, down, span):
    count = lax.axis_size("sp")
    quarter = down.shape[1]
    across = [[g * span + m for g in range(count // span)] for m in range(span)]
    both = lax.all_gather(
        both, "sp", axis_index_groups=across, tiled=True
    )
    down = lax.all_gather(down, "sp", axis_index_groups=across, tiled=True)
    down = jnp.transpose(down, (1, 0, 2)).reshape(quarter, -1)
    return both, down


def local(
    residual,
    values,
    gate_input,
    group_keys,
    time_step,
    decay_rate,
    skip_gain,
    conv_values,
    conv_keys,
    mix_gain,
    out_weight,
    norm_gain,
    hidden_gate,
    hidden_up,
    hidden_conv,
    hidden_down,
):
    row_count = values.shape[0]
    value_cols = values.shape[1]
    tap_count = conv_values.shape[0]
    sp_count = lax.axis_size("sp")
    span = min(SPAN, sp_count)
    member = lax.axis_index("sp") % span
    both_share, down_share = hidden_weights(hidden_gate, hidden_up, hidden_down, span)
    quarter = down_share.shape[1]
    tail_rows = jnp.concatenate(
        [values[row_count - tap_count + 1 :], group_keys[row_count - tap_count + 1 :]], axis=1
    )
    before_rows = from_behind(tail_rows, "sp", 1)
    before_rows, both_share, down_share = lax.optimization_barrier(
        (before_rows, both_share, down_share)
    )
    both_weights, down_quarter = gathered_weights(both_share, down_share, span)
    joined_values = jnp.concatenate([before_rows[:, :value_cols], values], axis=0).astype(
        jnp.float32
    )
    joined_keys = jnp.concatenate([before_rows[:, value_cols:], group_keys], axis=0).astype(
        jnp.float32
    )
    group_count = group_keys.shape[1] // (2 * STATE_WIDE + 2 * STATE_NARROW)
    inputs = jax.nn.silu(tap_sum(joined_values, conv_values, row_count)).reshape(
        row_count, group_count, GROUP_HEADS, HEAD_SIZE
    )
    key_rows = jax.nn.silu(tap_sum(joined_keys, conv_keys, row_count)).reshape(
        row_count, group_count, -1
    )
    deltas = jax.nn.softplus(time_step).T.reshape(row_count, group_count, GROUP_HEADS)
    rate_table = decay_rate.reshape(group_count, GROUP_HEADS)
    skip_table = skip_gain.reshape(group_count, GROUP_HEADS)
    running = jnp.cumsum(-rate_table * deltas, axis=0)
    half_heads = GROUP_HEADS // 2
    wide_end = 2 * STATE_WIDE

    def run_kind(head_first, head_last, key_first, state_width):
        in_keys = key_rows[..., key_first : key_first + state_width]
        out_keys = key_rows[..., key_first + state_width : key_first + 2 * state_width]
        carried = jnp.zeros(
            (group_count, head_last - head_first, HEAD_SIZE, state_width), jnp.float32
        )
        block_outs = []
        for block_index in range(row_count // BLOCK):
            row_first = block_index * BLOCK
            row_last = row_first + BLOCK
            block_out, carried = block_heads(
                inputs[row_first:row_last, :, head_first:head_last],
                in_keys[row_first:row_last],
                out_keys[row_first:row_last],
                deltas[row_first:row_last, :, head_first:head_last],
                rate_table[:, head_first:head_last],
                skip_table[:, head_first:head_last],
                carried,
            )
            block_outs.append(block_out)
        return (jnp.concatenate(block_outs, axis=0), carried, out_keys)

    wide_local, wide_state, wide_keys = run_kind(0, half_heads, 0, STATE_WIDE)
    narrow_local, narrow_state, narrow_keys = run_kind(
        half_heads, GROUP_HEADS, wide_end, STATE_NARROW
    )
    incoming = earlier_states(
        jnp.concatenate(
            [running[-1][:, :half_heads].reshape(-1), running[-1][:, half_heads:].reshape(-1)]
        ),
        (
            wide_state.reshape(-1, HEAD_SIZE, STATE_WIDE),
            narrow_state.reshape(-1, HEAD_SIZE, STATE_NARROW),
        ),
        "sp",
    )
    wide_in = incoming[0].reshape(wide_state.shape).astype(jnp.float32)
    narrow_in = incoming[1].reshape(narrow_state.shape).astype(jnp.float32)
    growth = jnp.exp(running)[..., None]
    wide_out = (
        wide_local
        + jnp.einsum("ign,ghpn->ighp", wide_keys, wide_in, precision=HIGHEST)
        * growth[:, :, :half_heads]
    )
    narrow_out = (
        narrow_local
        + jnp.einsum("ign,ghpn->ighp", narrow_keys, narrow_in, precision=HIGHEST)
        * growth[:, :, half_heads:]
    )
    mixer_out = jnp.concatenate([wide_out, narrow_out], axis=2).reshape(row_count, value_cols)
    gated_out = mixer_out * jax.nn.silu(gate_input.astype(jnp.float32))
    squares = lax.psum(jnp.sum(gated_out * gated_out, axis=1), "tp")
    inverse_rms = lax.rsqrt(squares / (value_cols * lax.axis_size("tp")) + NORM_FLOOR)
    gained = (gated_out * mix_gain).astype(jnp.bfloat16)
    mixer_part = lax.dot_general(
        out_weight, gained, (((0,), (1,)), ((), ())), preferred_element_type=jnp.float32
    ).astype(jnp.bfloat16)
    own_rows = residual.shape[0]
    mixer_sum = with_tp_sum(mixer_part, own_rows) * inverse_rms[None, :]
    own_merged = (residual.astype(jnp.float32) + mixer_sum).astype(jnp.bfloat16)
    pieces = [own_merged]
    for turn in range(1, span):
        pieces.append(from_member(own_merged, "sp", span, turn))
    mine = jnp.concatenate(pieces, axis=1)
    merged_wide = gathered_tp(mine).astype(jnp.float32)
    inverse_norm = lax.rsqrt(jnp.mean(merged_wide * merged_wide, axis=0) + NORM_FLOOR)
    lifted = (merged_wide * inverse_norm[None, :] * norm_gain[:, None]).astype(jnp.bfloat16)
    both_pre = contract_rows(both_weights, lifted).astype(jnp.bfloat16)
    edge_taps = hidden_conv.shape[1]
    both_pre = both_pre.reshape(2, quarter, span * row_count)
    ordered = [both_pre[:, :, j * row_count : (j + 1) * row_count] for j in range(span)]
    last_edges = [block[:, :, row_count - edge_taps + 1 :] for block in ordered]
    own_last = sum(
        jnp.where(member == (span - 1 + j) % span, 1, 0).astype(jnp.bfloat16) * last_edges[j]
        for j in range(span)
    )
    edge_before = from_behind(own_last, "sp", span)
    own_taps = lax.dynamic_slice_in_dim(hidden_conv, member * quarter, quarter, 2)
    hidden_blocks = []
    for j in range(span):
        first = member == j
        edge = jnp.where(first, edge_before, last_edges[(j + 1) % span])
        hidden_blocks.append(hidden_taps(ordered[j], edge, own_taps, row_count))
    hidden = jnp.concatenate(hidden_blocks, axis=1)
    down_part = contract_rows(down_quarter, hidden).astype(jnp.bfloat16)
    down_sum = with_tp_sum(down_part, own_rows)
    total = own_merged.astype(jnp.float32) + down_sum[:, :row_count]
    for turn in range(1, span):
        block = down_sum[:, turn * row_count : (turn + 1) * row_count].astype(jnp.bfloat16)
        total = total + from_member(block, "sp", span, span - turn).astype(jnp.float32)
    return total.astype(jnp.bfloat16)


def solution(mesh):
    in_specs = (
        P("tp", "sp"),
        P("sp", "tp"),
        P("sp", "tp"),
        P("sp", "tp"),
        P("tp", "sp"),
        P("tp"),
        P("tp"),
        P(None, "tp"),
        P(None, "tp"),
        P("tp"),
        P("tp", None),
        P(),
        P("sp", "tp"),
        P("sp", "tp"),
        P(None, None, "tp"),
        P("tp", "sp"),
    )
    out_specs = P("tp", "sp")
    return jax.shard_map(local, mesh=mesh, in_specs=in_specs, out_specs=out_specs, check_vma=False)
```

```python
import jax
import jax.numpy as jnp
from jax import lax
from jax.experimental import pallas as pl
from jax.experimental.pallas import tpu as pltpu
from jax.sharding import PartitionSpec as P

GROUP_HEADS = 8
HEAD_SIZE = 64
STATE_WIDE = 128
STATE_NARROW = 64
BLOCK = 128


NORM_FLOOR = 0.1
SPAN = 4
EDGE = 8
HIGHEST = lax.Precision.HIGHEST


def from_behind(value, axis, steps):
    count = lax.axis_size(axis)
    first, last = (max(0, -steps), min(count, count - steps))
    return lax.ppermute(value, axis, [(source, source + steps) for source in range(first, last)])


def earlier_states(log_spans, states, axis):
    count = lax.axis_size(axis)
    place = lax.axis_index(axis)
    slices = []
    for state in states:
        heads, size, width = state.shape
        cut = state.astype(jnp.bfloat16).reshape(heads, count, size // count * width)
        slices.append(jnp.transpose(cut, (1, 0, 2)).reshape(count, -1))
    split = slices[0].shape[1]
    high = lax.reduce_precision(log_spans, 8, 7)
    middle = lax.reduce_precision(log_spans - high, 8, 7)
    low = lax.reduce_precision(log_spans - high - middle, 8, 7)
    parts = jnp.concatenate([high, middle, low]).astype(jnp.bfloat16)
    slices.append(jnp.broadcast_to(parts, (count, parts.shape[0])))
    last = split + slices[1].shape[1]
    sent = jnp.concatenate(slices, axis=1)
    got = lax.all_to_all(sent, axis, split_axis=0, concat_axis=0, tiled=True)
    spans = got[:, last:].astype(jnp.float32).reshape(count, 3, -1).sum(axis=1)
    spot = jnp.arange(count)
    between = (spot[None, :, None] < spot) & (spot < spot[:, None, None])
    gaps = jnp.einsum("dsr,rh->dsh", between.astype(jnp.float32), spans, precision=HIGHEST)
    earlier = jnp.tril(jnp.ones((count, count), dtype=bool), -1)
    factors = jnp.exp(jnp.where(earlier[..., None], gaps, -jnp.inf))
    first = 0
    backs = []
    for state, part in zip(states, (got[:, :split], got[:, split:last])):
        heads, size, width = state.shape
        rows = part.reshape(count, heads, size // count * width)
        mine = factors[:, :, first : first + heads]
        first += heads
        backs.append(
            jnp.einsum("dsh,shn->dhn", mine.astype(jnp.bfloat16), rows, preferred_element_type=jnp.float32)
            .astype(jnp.bfloat16)
            .reshape(count, -1)
        )
    back = lax.all_to_all(
        jnp.concatenate(backs, axis=1), axis, split_axis=0, concat_axis=0, tiled=True
    )
    results = []
    for state, part in zip(states, (back[:, :split], back[:, split:])):
        heads, size, width = state.shape
        rows = part.reshape(count, heads, size // count, width)
        results.append(jnp.transpose(rows, (1, 0, 2, 3)).reshape(heads, size, width))
    return results


def from_member(shard, axis, span, turn):
    count = lax.axis_size(axis)
    return lax.ppermute(
        shard, axis, [(i, i - i % span + (i + turn) % span) for i in range(count)]
    )


def with_tp_sum(partial, rows):
    count = lax.axis_size("tp")
    place = lax.axis_index("tp")
    total = lax.dynamic_slice_in_dim(partial, place * rows, rows, 0).astype(jnp.float32)
    for turn in range(1, count):
        block = lax.dynamic_slice_in_dim(partial, (place + turn) % count * rows, rows, 0)
        total = total + from_member(block, "tp", count, turn).astype(jnp.float32)
    return total


def gathered_tp(mine):
    count = lax.axis_size("tp")
    if count > 2:
        return lax.all_gather(mine, "tp", axis=0, tiled=True)
    other = from_member(mine, "tp", count, 1)
    first = lax.axis_index("tp") == 0
    return jnp.concatenate([jnp.where(first, mine, other), jnp.where(first, other, mine)], axis=0)


def contract_rows(left, right):
    return lax.dot_general(
        left, right, (((0,), (0,)), ((), ())), preferred_element_type=jnp.float32
    )


def silu_taps(before, rows, taps):
    joined = jnp.concatenate([before.astype(jnp.float32), rows.astype(jnp.float32)], axis=0)
    count = rows.shape[0]
    first = before.shape[0] - taps.shape[0] + 1
    summed = taps[0:1].astype(jnp.float32) * joined[first : first + count]
    for tap in range(1, taps.shape[0]):
        summed = summed + taps[tap : tap + 1].astype(jnp.float32) * joined[
            first + tap : first + tap + count
        ]
    return summed * jax.nn.sigmoid(summed)


def local_heads(
    before_values, values, before_keys, keys, conv_values, conv_keys,
    run_row, run_col, delta_col, skip,
    local_out, wide_keys, narrow_keys, wide_state, narrow_state,
):
    count = values.shape[0]
    inputs = silu_taps(before_values[...], values[...], conv_values[...])
    key_rows = silu_taps(before_keys[...], keys[...], conv_keys[...]).astype(jnp.bfloat16)
    by_row, by_col, deltas = run_row[0], run_col[0], delta_col[0]
    below = lax.broadcasted_iota(jnp.int32, (count, count), 0) >= lax.broadcasted_iota(
        jnp.int32, (count, count), 1
    )
    half = GROUP_HEADS // 2
    outs = []
    for kind, (first, width, keys_out, state_out) in enumerate(
        ((0, STATE_WIDE, wide_keys, wide_state), (2 * STATE_WIDE, STATE_NARROW, narrow_keys, narrow_state))
    ):
        in_keys = key_rows[:, first : first + width]
        out_keys = key_rows[:, first + width : first + 2 * width]
        keys_out[0] = out_keys
        scores = lax.dot_general(
            out_keys, in_keys, (((1,), (1,)), ((), ())), preferred_element_type=jnp.float32
        )
        scaled = []
        for head in range(kind * half, (kind + 1) * half):
            gap = by_col[:, head : head + 1] - by_row[head : head + 1, :]
            mixing = (scores * jnp.exp(jnp.where(below, gap, -jnp.inf))).astype(jnp.bfloat16)
            own = slice(head * HEAD_SIZE, (head + 1) * HEAD_SIZE)
            weighted = inputs[:, own] * deltas[:, head : head + 1]
            outs.append(
                jnp.dot(mixing, weighted.astype(jnp.bfloat16), preferred_element_type=jnp.float32)
                + inputs[:, own] * skip[:, own]
            )
            to_end = jnp.exp(by_row[head : head + 1, count - 1 : count] - by_col[:, head : head + 1])
            scaled.append((weighted * to_end).astype(jnp.bfloat16))
        state_out[0] = lax.dot_general(
            jnp.concatenate(scaled, axis=1),
            in_keys,
            (((0,), (0,)), ((), ())),
            preferred_element_type=jnp.float32,
        ).astype(jnp.bfloat16)
    local_out[...] = jnp.concatenate(outs, axis=1)


def carried_heads(
    local_out, wide_keys, narrow_keys, wide_in, narrow_in, run_col, gates, gain, gained, squares
):
    half = GROUP_HEADS // 2
    growth = jnp.exp(run_col[0])
    parts = []
    for kind, (keys, state) in enumerate(((wide_keys, wide_in), (narrow_keys, narrow_in))):
        read = lax.dot_general(
            keys[0], state[0], (((1,), (1,)), ((), ())), preferred_element_type=jnp.float32
        )
        for spot in range(half):
            head = kind * half + spot
            parts.append(
                read[:, spot * HEAD_SIZE : (spot + 1) * HEAD_SIZE] * growth[:, head : head + 1]
            )
    gate = gates[...].astype(jnp.float32)
    gated = (local_out[...] + jnp.concatenate(parts, axis=1)) * (gate * jax.nn.sigmoid(gate))
    squares[0] = jnp.sum(gated * gated, axis=1, keepdims=True)
    gained[...] = (gated * gain[...]).astype(jnp.bfloat16)


def by_group(*shape):
    return pl.BlockSpec((1,) + shape, lambda g: (g, 0, 0))


def by_cols(rows, cols):
    return pl.BlockSpec((rows, cols), lambda g: (0, g))


def hidden_taps(both_pre, edge_cols, taps, row_count):
    joined_hidden = jnp.concatenate([edge_cols, both_pre], axis=2).astype(jnp.float32)
    conv_total = taps[:, 0, :, None].astype(jnp.float32) * joined_hidden[:, :, 0:row_count]
    for tap_index in range(1, taps.shape[1]):
        conv_total = (
            conv_total
            + taps[:, tap_index, :, None].astype(jnp.float32)
            * joined_hidden[:, :, tap_index : tap_index + row_count]
        )
    return (jax.nn.silu(conv_total[0]) * conv_total[1]).astype(jnp.bfloat16)


def hidden_weights(hidden_gate, hidden_up, hidden_down, span):
    count = lax.axis_size("sp")
    rows, hidden_cols = hidden_gate.shape
    quarter = hidden_cols // span
    within = [[g * span + m for m in range(span)] for g in range(count // span)]
    gates = hidden_gate.reshape(rows, span, quarter)
    ups = hidden_up.reshape(rows, span, quarter)
    both = jnp.transpose(jnp.concatenate([gates, ups], axis=2), (1, 0, 2))
    down = hidden_down.reshape(span, quarter, hidden_down.shape[1])
    both = lax.all_to_all(both, "sp", 0, 0, axis_index_groups=within, tiled=True)
    down = lax.all_to_all(down, "sp", 0, 0, axis_index_groups=within, tiled=True)
    return both.reshape(span * rows, 2 * quarter), down


def across_spans(share, span):
    count = lax.axis_size("sp")
    across = [[g * span + m for g in range(count // span)] for m in range(span)]
    return lax.all_gather(share, "sp", axis_index_groups=across, tiled=True)


def local(
    residual,
    values,
    gate_input,
    group_keys,
    time_step,
    decay_rate,
    skip_gain,
    conv_values,
    conv_keys,
    mix_gain,
    out_weight,
    norm_gain,
    hidden_gate,
    hidden_up,
    hidden_conv,
    hidden_down,
):
    row_count = values.shape[0]
    value_cols = values.shape[1]
    tap_count = conv_values.shape[0]
    sp_count = lax.axis_size("sp")
    span = min(SPAN, sp_count)
    member = lax.axis_index("sp") % span
    both_share, down_share = hidden_weights(hidden_gate, hidden_up, hidden_down, span)
    quarter = down_share.shape[1]
    tail_rows = jnp.concatenate([values[row_count - EDGE :], group_keys[row_count - EDGE :]], axis=1)
    before_rows = from_behind(tail_rows, "sp", 1)
    before_rows, both_share = lax.optimization_barrier((before_rows, both_share))
    both_weights = across_spans(both_share, span)
    group_keys_cols = 2 * STATE_WIDE + 2 * STATE_NARROW
    group_count = group_keys.shape[1] // group_keys_cols
    group_cols = GROUP_HEADS * HEAD_SIZE
    half_rows = group_cols // 2
    deltas = jax.nn.softplus(time_step)
    running = jnp.cumsum(-decay_rate[:, None] * deltas, axis=1)
    run_row = running.reshape(group_count, GROUP_HEADS, row_count)
    run_col = jnp.transpose(run_row, (0, 2, 1))
    delta_col = jnp.transpose(deltas.reshape(group_count, GROUP_HEADS, row_count), (0, 2, 1))
    skip = jnp.repeat(skip_gain, HEAD_SIZE)[None, :]
    local_out, wide_keys, narrow_keys, wide_state, narrow_state = pl.pallas_call(
        local_heads,
        grid=(group_count,),
        in_specs=[
            by_cols(EDGE, group_cols),
            by_cols(row_count, group_cols),
            by_cols(EDGE, group_keys_cols),
            by_cols(row_count, group_keys_cols),
            by_cols(tap_count, group_cols),
            by_cols(tap_count, group_keys_cols),
            by_group(GROUP_HEADS, row_count),
            by_group(row_count, GROUP_HEADS),
            by_group(row_count, GROUP_HEADS),
            by_cols(1, group_cols),
        ],
        out_specs=[
            by_cols(row_count, group_cols),
            by_group(row_count, STATE_WIDE),
            by_group(row_count, STATE_NARROW),
            by_group(half_rows, STATE_WIDE),
            by_group(half_rows, STATE_NARROW),
        ],
        out_shape=[
            jax.ShapeDtypeStruct((row_count, value_cols), jnp.float32),
            jax.ShapeDtypeStruct((group_count, row_count, STATE_WIDE), jnp.bfloat16),
            jax.ShapeDtypeStruct((group_count, row_count, STATE_NARROW), jnp.bfloat16),
            jax.ShapeDtypeStruct((group_count, half_rows, STATE_WIDE), jnp.bfloat16),
            jax.ShapeDtypeStruct((group_count, half_rows, STATE_NARROW), jnp.bfloat16),
        ],
        cost_estimate=pl.CostEstimate(flops=10**9, bytes_accessed=10**7, transcendentals=10**6),
        name="local_heads",
    )(
        before_rows[:, :value_cols],
        values,
        before_rows[:, value_cols:],
        group_keys,
        conv_values,
        conv_keys,
        run_row,
        run_col,
        delta_col,
        skip,
    )
    spans = run_row[:, :, -1]
    half_heads = GROUP_HEADS // 2
    incoming = earlier_states(
        jnp.concatenate(
            [spans[:, :half_heads].reshape(-1), spans[:, half_heads:].reshape(-1)]
        ),
        (
            wide_state.reshape(-1, HEAD_SIZE, STATE_WIDE),
            narrow_state.reshape(-1, HEAD_SIZE, STATE_NARROW),
        ),
        "sp",
    )
    incoming[0], down_share = lax.optimization_barrier((incoming[0], down_share))
    down_quarter = across_spans(down_share, span)
    gained, squares = pl.pallas_call(
        carried_heads,
        grid=(group_count,),
        in_specs=[
            by_cols(row_count, group_cols),
            by_group(row_count, STATE_WIDE),
            by_group(row_count, STATE_NARROW),
            by_group(half_rows, STATE_WIDE),
            by_group(half_rows, STATE_NARROW),
            by_group(row_count, GROUP_HEADS),
            by_cols(row_count, group_cols),
            by_cols(1, group_cols),
        ],
        out_specs=[by_cols(row_count, group_cols), by_group(row_count, 1)],
        out_shape=[
            jax.ShapeDtypeStruct((row_count, value_cols), jnp.bfloat16),
            jax.ShapeDtypeStruct((group_count, row_count, 1), jnp.float32),
        ],
        cost_estimate=pl.CostEstimate(flops=10**8, bytes_accessed=10**7, transcendentals=10**6),
        name="carried_heads",
    )(
        local_out,
        wide_keys,
        narrow_keys,
        incoming[0].reshape(wide_state.shape),
        incoming[1].reshape(narrow_state.shape),
        run_col,
        gate_input,
        mix_gain[None, :],
    )
    squares = lax.psum(jnp.sum(squares[:, :, 0], axis=0), "tp")
    inverse_rms = lax.rsqrt(squares / (value_cols * lax.axis_size("tp")) + NORM_FLOOR)
    mixer_part = lax.dot_general(
        out_weight, gained, (((0,), (1,)), ((), ())), preferred_element_type=jnp.float32
    ).astype(jnp.bfloat16)
    own_rows = residual.shape[0]
    mixer_sum = with_tp_sum(mixer_part, own_rows) * inverse_rms[None, :]
    own_merged = (residual.astype(jnp.float32) + mixer_sum).astype(jnp.bfloat16)
    pieces = [own_merged]
    for turn in range(1, span):
        pieces.append(from_member(own_merged, "sp", span, turn))
    mine = jnp.concatenate(pieces, axis=1)
    merged_wide = gathered_tp(mine).astype(jnp.float32)
    inverse_norm = lax.rsqrt(jnp.mean(merged_wide * merged_wide, axis=0) + NORM_FLOOR)
    lifted = (merged_wide * inverse_norm[None, :] * norm_gain[:, None]).astype(jnp.bfloat16)
    both_pre = contract_rows(both_weights, lifted).astype(jnp.bfloat16)
    edge_taps = hidden_conv.shape[1]
    both_pre = both_pre.reshape(2, quarter, span * row_count)
    ordered = [both_pre[:, :, j * row_count : (j + 1) * row_count] for j in range(span)]
    last_edges = [block[:, :, row_count - edge_taps + 1 :] for block in ordered]
    own_last = sum(
        jnp.where(member == (span - 1 + j) % span, 1, 0).astype(jnp.bfloat16) * last_edges[j]
        for j in range(span)
    )
    edge_before = from_behind(own_last, "sp", span)
    own_taps = lax.dynamic_slice_in_dim(hidden_conv, member * quarter, quarter, 2)
    hidden_blocks = []
    for j in range(span):
        first = member == j
        edge = jnp.where(first, edge_before, last_edges[(j + 1) % span])
        hidden_blocks.append(hidden_taps(ordered[j], edge, own_taps, row_count))
    hidden = jnp.concatenate(hidden_blocks, axis=1)
    hidden, down_quarter = lax.optimization_barrier((hidden, down_quarter))
    down_quarter = jnp.transpose(
        down_quarter.reshape(-1, quarter, down_share.shape[2]), (1, 0, 2)
    ).reshape(quarter, -1)
    down_part = contract_rows(down_quarter, hidden).astype(jnp.bfloat16)
    down_sum = with_tp_sum(down_part, own_rows)
    total = own_merged.astype(jnp.float32) + down_sum[:, :row_count]
    for turn in range(1, span):
        block = down_sum[:, turn * row_count : (turn + 1) * row_count].astype(jnp.bfloat16)
        total = total + from_member(block, "sp", span, span - turn).astype(jnp.float32)
    return total.astype(jnp.bfloat16)


def solution(mesh):
    in_specs = (
        P("tp", "sp"),
        P("sp", "tp"),
        P("sp", "tp"),
        P("sp", "tp"),
        P("tp", "sp"),
        P("tp"),
        P("tp"),
        P(None, "tp"),
        P(None, "tp"),
        P("tp"),
        P("tp", None),
        P(),
        P("sp", "tp"),
        P("sp", "tp"),
        P(None, None, "tp"),
        P("tp", "sp"),
    )
    out_specs = P("tp", "sp")
    return jax.shard_map(local, mesh=mesh, in_specs=in_specs, out_specs=out_specs, check_vma=False)
```

```python
import jax
import jax.numpy as jnp
from jax import lax
from jax.experimental import pallas as pl
from jax.experimental.pallas import tpu as pltpu
from jax.sharding import PartitionSpec as P

GROUP_HEADS = 8
HEAD_SIZE = 64
STATE_WIDE = 128
STATE_NARROW = 64
BLOCK = 128


NORM_FLOOR = 0.1
SPAN = 4
EDGE = 8
HIGHEST = lax.Precision.HIGHEST


def from_behind(value, axis, steps):
    count = lax.axis_size(axis)
    first, last = (max(0, -steps), min(count, count - steps))
    return lax.ppermute(value, axis, [(source, source + steps) for source in range(first, last)])


def earlier_states(log_spans, states, axis):
    count = lax.axis_size(axis)
    place = lax.axis_index(axis)
    slices = []
    for state in states:
        heads, size, width = state.shape
        cut = state.astype(jnp.bfloat16).reshape(heads, count, size // count * width)
        slices.append(jnp.transpose(cut, (1, 0, 2)).reshape(count, -1))
    split = slices[0].shape[1]
    high = lax.reduce_precision(log_spans, 8, 7)
    middle = lax.reduce_precision(log_spans - high, 8, 7)
    low = lax.reduce_precision(log_spans - high - middle, 8, 7)
    parts = jnp.concatenate([high, middle, low]).astype(jnp.bfloat16)
    slices.append(jnp.broadcast_to(parts, (count, parts.shape[0])))
    last = split + slices[1].shape[1]
    sent = jnp.concatenate(slices, axis=1)
    got = lax.all_to_all(sent, axis, split_axis=0, concat_axis=0, tiled=True)
    spans = got[:, last:].astype(jnp.float32).reshape(count, 3, -1).sum(axis=1)
    spot = jnp.arange(count)
    between = (spot[None, :, None] < spot) & (spot < spot[:, None, None])
    gaps = jnp.einsum("dsr,rh->dsh", between.astype(jnp.float32), spans, precision=HIGHEST)
    earlier = jnp.tril(jnp.ones((count, count), dtype=bool), -1)
    factors = jnp.exp(jnp.where(earlier[..., None], gaps, -jnp.inf))
    first = 0
    backs = []
    for state, part in zip(states, (got[:, :split], got[:, split:last])):
        heads, size, width = state.shape
        rows = part.reshape(count, heads, size // count * width)
        mine = factors[:, :, first : first + heads]
        first += heads
        backs.append(
            jnp.einsum("dsh,shn->dhn", mine.astype(jnp.bfloat16), rows, preferred_element_type=jnp.float32)
            .astype(jnp.bfloat16)
            .reshape(count, -1)
        )
    back = lax.all_to_all(
        jnp.concatenate(backs, axis=1), axis, split_axis=0, concat_axis=0, tiled=True
    )
    results = []
    for state, part in zip(states, (back[:, :split], back[:, split:])):
        heads, size, width = state.shape
        rows = part.reshape(count, heads, size // count, width)
        results.append(jnp.transpose(rows, (1, 0, 2, 3)).reshape(heads, size, width))
    return results


def from_member(shard, axis, span, turn):
    count = lax.axis_size(axis)
    return lax.ppermute(
        shard, axis, [(i, i - i % span + (i + turn) % span) for i in range(count)]
    )


def with_tp_sum(partial, rows):
    count = lax.axis_size("tp")
    place = lax.axis_index("tp")
    total = lax.dynamic_slice_in_dim(partial, place * rows, rows, 0).astype(jnp.float32)
    for turn in range(1, count):
        block = lax.dynamic_slice_in_dim(partial, (place + turn) % count * rows, rows, 0)
        total = total + from_member(block, "tp", count, turn).astype(jnp.float32)
    return total


def gathered_tp(mine):
    count = lax.axis_size("tp")
    if count > 2:
        return lax.all_gather(mine, "tp", axis=0, tiled=True)
    other = from_member(mine, "tp", count, 1)
    first = lax.axis_index("tp") == 0
    return jnp.concatenate([jnp.where(first, mine, other), jnp.where(first, other, mine)], axis=0)


def contract_rows(left, right):
    return lax.dot_general(
        left, right, (((0,), (0,)), ((), ())), preferred_element_type=jnp.float32
    )


def silu_taps(before, rows, taps):
    joined = jnp.concatenate([before.astype(jnp.float32), rows.astype(jnp.float32)], axis=0)
    count = rows.shape[0]
    first = before.shape[0] - taps.shape[0] + 1
    summed = taps[0:1].astype(jnp.float32) * joined[first : first + count]
    for tap in range(1, taps.shape[0]):
        summed = summed + taps[tap : tap + 1].astype(jnp.float32) * joined[
            first + tap : first + tap + count
        ]
    return summed * jax.nn.sigmoid(summed)


def local_heads(
    before_values, values, before_keys, keys, conv_values, conv_keys,
    run_row, run_col, delta_col, skip,
    local_out, wide_keys, narrow_keys, wide_state, narrow_state,
):
    count = values.shape[0]
    inputs = silu_taps(before_values[...], values[...], conv_values[...])
    key_rows = silu_taps(before_keys[...], keys[...], conv_keys[...]).astype(jnp.bfloat16)
    by_row, by_col, deltas = run_row[0], run_col[0], delta_col[0]
    below = lax.broadcasted_iota(jnp.int32, (count, count), 0) >= lax.broadcasted_iota(
        jnp.int32, (count, count), 1
    )
    half = GROUP_HEADS // 2
    outs = []
    for kind, (first, width, keys_out, state_out) in enumerate(
        ((0, STATE_WIDE, wide_keys, wide_state), (2 * STATE_WIDE, STATE_NARROW, narrow_keys, narrow_state))
    ):
        in_keys = key_rows[:, first : first + width]
        out_keys = key_rows[:, first + width : first + 2 * width]
        keys_out[0] = out_keys
        scores = lax.dot_general(
            out_keys, in_keys, (((1,), (1,)), ((), ())), preferred_element_type=jnp.float32
        )
        scaled = []
        for head in range(kind * half, (kind + 1) * half):
            gap = by_col[:, head : head + 1] - by_row[head : head + 1, :]
            mixing = (scores * jnp.exp(jnp.where(below, gap, -jnp.inf))).astype(jnp.bfloat16)
            own = slice(head * HEAD_SIZE, (head + 1) * HEAD_SIZE)
            weighted = inputs[:, own] * deltas[:, head : head + 1]
            outs.append(
                jnp.dot(mixing, weighted.astype(jnp.bfloat16), preferred_element_type=jnp.float32)
                + inputs[:, own] * skip[:, own]
            )
            to_end = jnp.exp(by_row[head : head + 1, count - 1 : count] - by_col[:, head : head + 1])
            scaled.append((weighted * to_end).astype(jnp.bfloat16))
        state_out[0] = lax.dot_general(
            jnp.concatenate(scaled, axis=1),
            in_keys,
            (((0,), (0,)), ((), ())),
            preferred_element_type=jnp.float32,
        ).astype(jnp.bfloat16)
    local_out[...] = jnp.concatenate(outs, axis=1)


def carried_heads(
    local_out, wide_keys, narrow_keys, wide_in, narrow_in, run_col, gates, gain, gained, squares
):
    half = GROUP_HEADS // 2
    growth = jnp.exp(run_col[0])
    parts = []
    for kind, (keys, state) in enumerate(((wide_keys, wide_in), (narrow_keys, narrow_in))):
        read = lax.dot_general(
            keys[0], state[0], (((1,), (1,)), ((), ())), preferred_element_type=jnp.float32
        )
        for spot in range(half):
            head = kind * half + spot
            parts.append(
                read[:, spot * HEAD_SIZE : (spot + 1) * HEAD_SIZE] * growth[:, head : head + 1]
            )
    gate = gates[...].astype(jnp.float32)
    gated = (local_out[...] + jnp.concatenate(parts, axis=1)) * (gate * jax.nn.sigmoid(gate))
    squares[0] = jnp.sum(gated * gated, axis=1, keepdims=True)
    gained[...] = (gated * gain[...]).astype(jnp.bfloat16)


def by_group(*shape):
    return pl.BlockSpec((1,) + shape, lambda g: (g, 0, 0))


def by_cols(rows, cols):
    return pl.BlockSpec((rows, cols), lambda g: (0, g))


def hidden_taps(both_pre, edge_cols, taps, row_count):
    joined_hidden = jnp.concatenate([edge_cols, both_pre], axis=2).astype(jnp.float32)
    conv_total = taps[:, 0, :, None].astype(jnp.float32) * joined_hidden[:, :, 0:row_count]
    for tap_index in range(1, taps.shape[1]):
        conv_total = (
            conv_total
            + taps[:, tap_index, :, None].astype(jnp.float32)
            * joined_hidden[:, :, tap_index : tap_index + row_count]
        )
    return (jax.nn.silu(conv_total[0]) * conv_total[1]).astype(jnp.bfloat16)


def hidden_weights(hidden_gate, hidden_up, hidden_down, span):
    count = lax.axis_size("sp")
    rows, hidden_cols = hidden_gate.shape
    quarter = hidden_cols // span
    within = [[g * span + m for m in range(span)] for g in range(count // span)]
    gates = hidden_gate.reshape(rows, span, quarter)
    ups = hidden_up.reshape(rows, span, quarter)
    both = jnp.transpose(jnp.concatenate([gates, ups], axis=2), (1, 0, 2))
    down = hidden_down.reshape(span, quarter, hidden_down.shape[1])
    both = lax.all_to_all(both, "sp", 0, 0, axis_index_groups=within, tiled=True)
    down = lax.all_to_all(down, "sp", 0, 0, axis_index_groups=within, tiled=True)
    return both.reshape(span * rows, 2 * quarter), down


def across_spans(share, span):
    count = lax.axis_size("sp")
    across = [[g * span + m for g in range(count // span)] for m in range(span)]
    return lax.all_gather(share, "sp", axis_index_groups=across, tiled=True)


def local(
    residual,
    values,
    gate_input,
    group_keys,
    time_step,
    decay_rate,
    skip_gain,
    conv_values,
    conv_keys,
    mix_gain,
    out_weight,
    norm_gain,
    hidden_gate,
    hidden_up,
    hidden_conv,
    hidden_down,
):
    row_count = values.shape[0]
    value_cols = values.shape[1]
    tap_count = conv_values.shape[0]
    sp_count = lax.axis_size("sp")
    span = min(SPAN, sp_count)
    member = lax.axis_index("sp") % span
    both_share, down_share = hidden_weights(hidden_gate, hidden_up, hidden_down, span)
    quarter = down_share.shape[1]
    tail_rows = jnp.concatenate([values[row_count - EDGE :], group_keys[row_count - EDGE :]], axis=1)
    before_rows = from_behind(tail_rows, "sp", 1)
    before_rows, both_share = lax.optimization_barrier((before_rows, both_share))
    both_weights = across_spans(both_share, span)
    group_keys_cols = 2 * STATE_WIDE + 2 * STATE_NARROW
    group_count = group_keys.shape[1] // group_keys_cols
    group_cols = GROUP_HEADS * HEAD_SIZE
    half_rows = group_cols // 2
    deltas = jax.nn.softplus(time_step)
    running = jnp.cumsum(-decay_rate[:, None] * deltas, axis=1)
    run_row = running.reshape(group_count, GROUP_HEADS, row_count)
    run_col = jnp.transpose(run_row, (0, 2, 1))
    delta_col = jnp.transpose(deltas.reshape(group_count, GROUP_HEADS, row_count), (0, 2, 1))
    skip = jnp.repeat(skip_gain, HEAD_SIZE)[None, :]
    local_out, wide_keys, narrow_keys, wide_state, narrow_state = pl.pallas_call(
        local_heads,
        grid=(group_count,),
        in_specs=[
            by_cols(EDGE, group_cols),
            by_cols(row_count, group_cols),
            by_cols(EDGE, group_keys_cols),
            by_cols(row_count, group_keys_cols),
            by_cols(tap_count, group_cols),
            by_cols(tap_count, group_keys_cols),
            by_group(GROUP_HEADS, row_count),
            by_group(row_count, GROUP_HEADS),
            by_group(row_count, GROUP_HEADS),
            by_cols(1, group_cols),
        ],
        out_specs=[
            by_cols(row_count, group_cols),
            by_group(row_count, STATE_WIDE),
            by_group(row_count, STATE_NARROW),
            by_group(half_rows, STATE_WIDE),
            by_group(half_rows, STATE_NARROW),
        ],
        out_shape=[
            jax.ShapeDtypeStruct((row_count, value_cols), jnp.float32),
            jax.ShapeDtypeStruct((group_count, row_count, STATE_WIDE), jnp.bfloat16),
            jax.ShapeDtypeStruct((group_count, row_count, STATE_NARROW), jnp.bfloat16),
            jax.ShapeDtypeStruct((group_count, half_rows, STATE_WIDE), jnp.bfloat16),
            jax.ShapeDtypeStruct((group_count, half_rows, STATE_NARROW), jnp.bfloat16),
        ],
        cost_estimate=pl.CostEstimate(flops=10**9, bytes_accessed=10**7, transcendentals=10**6),
        name="local_heads",
    )(
        before_rows[:, :value_cols],
        values,
        before_rows[:, value_cols:],
        group_keys,
        conv_values,
        conv_keys,
        run_row,
        run_col,
        delta_col,
        skip,
    )
    wide_state, down_share = lax.optimization_barrier((wide_state, down_share))
    down_quarter = across_spans(down_share, span)
    spans = run_row[:, :, -1]
    half_heads = GROUP_HEADS // 2
    incoming = earlier_states(
        jnp.concatenate(
            [spans[:, :half_heads].reshape(-1), spans[:, half_heads:].reshape(-1)]
        ),
        (
            wide_state.reshape(-1, HEAD_SIZE, STATE_WIDE),
            narrow_state.reshape(-1, HEAD_SIZE, STATE_NARROW),
        ),
        "sp",
    )
    gained, squares = pl.pallas_call(
        carried_heads,
        grid=(group_count,),
        in_specs=[
            by_cols(row_count, group_cols),
            by_group(row_count, STATE_WIDE),
            by_group(row_count, STATE_NARROW),
            by_group(half_rows, STATE_WIDE),
            by_group(half_rows, STATE_NARROW),
            by_group(row_count, GROUP_HEADS),
            by_cols(row_count, group_cols),
            by_cols(1, group_cols),
        ],
        out_specs=[by_cols(row_count, group_cols), by_group(row_count, 1)],
        out_shape=[
            jax.ShapeDtypeStruct((row_count, value_cols), jnp.bfloat16),
            jax.ShapeDtypeStruct((group_count, row_count, 1), jnp.float32),
        ],
        cost_estimate=pl.CostEstimate(flops=10**8, bytes_accessed=10**7, transcendentals=10**6),
        name="carried_heads",
    )(
        local_out,
        wide_keys,
        narrow_keys,
        incoming[0].reshape(wide_state.shape),
        incoming[1].reshape(narrow_state.shape),
        run_col,
        gate_input,
        mix_gain[None, :],
    )
    squares = lax.psum(jnp.sum(squares[:, :, 0], axis=0), "tp")
    inverse_rms = lax.rsqrt(squares / (value_cols * lax.axis_size("tp")) + NORM_FLOOR)
    mixer_part = lax.dot_general(
        out_weight, gained, (((0,), (1,)), ((), ())), preferred_element_type=jnp.float32
    ).astype(jnp.bfloat16)
    own_rows = residual.shape[0]
    mixer_sum = with_tp_sum(mixer_part, own_rows) * inverse_rms[None, :]
    own_merged = (residual.astype(jnp.float32) + mixer_sum).astype(jnp.bfloat16)
    pieces = [own_merged]
    for turn in range(1, span):
        pieces.append(from_member(own_merged, "sp", span, turn))
    mine = jnp.concatenate(pieces, axis=1)
    merged_wide = gathered_tp(mine).astype(jnp.float32)
    inverse_norm = lax.rsqrt(jnp.mean(merged_wide * merged_wide, axis=0) + NORM_FLOOR)
    lifted = (merged_wide * inverse_norm[None, :] * norm_gain[:, None]).astype(jnp.bfloat16)
    both_pre = contract_rows(both_weights, lifted).astype(jnp.bfloat16)
    edge_taps = hidden_conv.shape[1]
    both_pre = both_pre.reshape(2, quarter, span * row_count)
    ordered = [both_pre[:, :, j * row_count : (j + 1) * row_count] for j in range(span)]
    last_edges = [block[:, :, row_count - edge_taps + 1 :] for block in ordered]
    own_last = sum(
        jnp.where(member == (span - 1 + j) % span, 1, 0).astype(jnp.bfloat16) * last_edges[j]
        for j in range(span)
    )
    edge_before = from_behind(own_last, "sp", span)
    own_taps = lax.dynamic_slice_in_dim(hidden_conv, member * quarter, quarter, 2)
    hidden_blocks = []
    for j in range(span):
        first = member == j
        edge = jnp.where(first, edge_before, last_edges[(j + 1) % span])
        hidden_blocks.append(hidden_taps(ordered[j], edge, own_taps, row_count))
    hidden = jnp.concatenate(hidden_blocks, axis=1)
    hidden, down_quarter = lax.optimization_barrier((hidden, down_quarter))
    down_quarter = jnp.transpose(
        down_quarter.reshape(-1, quarter, down_share.shape[2]), (1, 0, 2)
    ).reshape(quarter, -1)
    down_part = contract_rows(down_quarter, hidden).astype(jnp.bfloat16)
    down_sum = with_tp_sum(down_part, own_rows)
    total = own_merged.astype(jnp.float32) + down_sum[:, :row_count]
    for turn in range(1, span):
        block = down_sum[:, turn * row_count : (turn + 1) * row_count].astype(jnp.bfloat16)
        total = total + from_member(block, "sp", span, span - turn).astype(jnp.float32)
    return total.astype(jnp.bfloat16)


def solution(mesh):
    in_specs = (
        P("tp", "sp"),
        P("sp", "tp"),
        P("sp", "tp"),
        P("sp", "tp"),
        P("tp", "sp"),
        P("tp"),
        P("tp"),
        P(None, "tp"),
        P(None, "tp"),
        P("tp"),
        P("tp", None),
        P(),
        P("sp", "tp"),
        P("sp", "tp"),
        P(None, None, "tp"),
        P("tp", "sp"),
    )
    out_specs = P("tp", "sp")
    return jax.shard_map(local, mesh=mesh, in_specs=in_specs, out_specs=out_specs, check_vma=False)
```
